32 devices in a mesh: sp: 8 (over z, y), tp: 4 (over x, core).
Axes of the slice: x: 2, y: 2, z: 4, core: 2. Of those that a mesh axis runs over, the one named last changes fastest.
Arguments:
- residual: bfloat16 [3072, 2048], P('sp'), may hold values from -50 to 50
- queries_a: bfloat16 [3072, 512], P('sp', 'tp'), may hold values from -50 to 50
- keys_a: bfloat16 [3072, 512], P('sp', 'tp'), may hold values from -9 to 9
- values_a: bfloat16 [3072, 512], P('sp', 'tp'), may hold values from -6 to 6
- queries_b: bfloat16 [3072, 1024], P('sp', 'tp'), may hold values from -50 to 50
- keys_b: bfloat16 [3072, 1024], P('sp', 'tp'), may hold values from -9 to 9
- values_b: bfloat16 [3072, 512], P('sp', 'tp'), may hold values from -6 to 6
- mix_lambda: float32 [2, 4], P(None, 'tp'), may hold values from 0.3 to 0.8
- head_gain: float32 [2, 128], replicated, may hold values from 0.1 to 1.9
- out_a: bfloat16 [512, 2048], P('tp'), may hold values from -0.1875 to 0.1875
- out_b: bfloat16 [512, 2048], P('tp'), may hold values from -0.1875 to 0.1875
- norm_gain: float32 [2048], replicated, may hold values from 0.1 to 1.9
- w_gate: bfloat16 [2048, 5632], P('sp', 'tp'), may hold values from -0.125 to 0.125
- w_up: bfloat16 [2048, 5632], P('sp', 'tp'), may hold values from -0.125 to 0.125
- w_down: bfloat16 [5632, 2048], P('tp', 'sp'), may hold values from -0.21875 to 0.21875
Outputs:
- layer_out: bfloat16 [3072, 2048], P('sp', 'tp')
The draws below stay inside these ranges and needn't reach their ends.
All inputs are finite; a program needn't handle non-finite values.
Results may differ from the reference program's by a relative error of at most 0.0085.
Values may be sent and summed in bfloat16 or wider, within the bound.
A program may use at most 256 MiB of HBM per device.

```python
import math
import jax
import jax.numpy as jnp
from jax import lax

D = 2048
FF = 5632
HEADS = 4
QA = 64
QB = 128
VD = 128
TOKENS = 3072


def draw_residual(key, part):
    base = jax.random.fold_in(key, 3)
    first, second = jax.random.split(base, 2)
    column = jnp.arange(D, dtype=jnp.float32) / D
    noise = jnp.clip(jax.random.normal(first, (TOKENS, D), jnp.float32), -6.0, 6.0)
    columns = 0.4 * 10.0 ** column
    row_scale = 2.0 ** jax.random.uniform(second, (TOKENS, 1), jnp.float32, -1.0, 1.0)
    return (noise * columns[None, :] * row_scale).astype(jnp.bfloat16)


def paired(key, width, salt):
    base = jax.random.fold_in(key, salt)
    query_seed, key_seed = jax.random.split(base, 2)
    columns = HEADS * 2 * width
    queries = 1.3 * jnp.clip(jax.random.normal(query_seed, (TOKENS, columns), jnp.float32), -6.0, 6.0)
    keys = 1.3 * jnp.clip(jax.random.normal(key_seed, (TOKENS, columns), jnp.float32), -6.0, 6.0)
    return (queries, keys)


def draw_queries_a(key, part):
    return paired(key, QA, 11)[0].astype(jnp.bfloat16)


def draw_keys_a(key, part):
    return paired(key, QA, 11)[1].astype(jnp.bfloat16)


def draw_queries_b(key, part):
    return paired(key, QB, 13)[0].astype(jnp.bfloat16)


def draw_keys_b(key, part):
    return paired(key, QB, 13)[1].astype(jnp.bfloat16)


def block_scale(rng, extent, pieces, least, largest):
    def one(position, blocks):
        draws = jax.random.uniform(jax.random.fold_in(jax.random.fold_in(rng, 6), position), (blocks,), jnp.float32, least / len(pieces), largest / len(pieces))
        return jnp.repeat(jnp.exp(draws), extent[position] // blocks).reshape((-1,) + (1,) * (len(extent) - position - 1))

    level = one(*pieces[0])
    for cut in pieces[1:]:
        level = level * one(*cut)
    return level


def scatter_about(key, shape, scale, limit, cuts=(), kind=jnp.bfloat16):
    level = block_scale(key, shape, cuts, -0.22, 0.18) if cuts else 1.0
    values = jax.random.normal(key, shape, jnp.float32) * scale * level
    return jnp.minimum(jnp.maximum(values, -limit), limit).astype(kind)


def setup_inputs(seed: int = 0) -> dict:
    streams_of = jax.random.split(jax.random.key(seed), 16)
    return {
        "residual": draw_residual(jax.random.fold_in(streams_of[15], 71), 0),
        "queries_a": draw_queries_a(jax.random.fold_in(streams_of[15], 71), 0),
        "keys_a": draw_keys_a(jax.random.fold_in(streams_of[15], 71), 0),
        "values_a": scatter_about(streams_of[3], (TOKENS, HEADS * VD), 1.0, 6.0, ((0, 8), (1, 4))),
        "queries_b": draw_queries_b(jax.random.fold_in(streams_of[15], 71), 0),
        "keys_b": draw_keys_b(jax.random.fold_in(streams_of[15], 71), 0),
        "values_b": scatter_about(streams_of[6], (TOKENS, HEADS * VD), 1.0, 6.0, ((0, 8), (1, 4))),
        "mix_lambda": jnp.clip(0.3 + 0.5 * jax.random.uniform(streams_of[7], (2, HEADS), jnp.float32) ** block_scale(streams_of[7], (2, HEADS), ((1, 4),), -0.2, 0.2), 0.3, 0.8),
        "head_gain": jnp.clip(1.0 + 0.18 * jax.random.normal(streams_of[8], (2, VD), jnp.float32), 0.1, 1.9),
        "out_a": scatter_about(streams_of[9], (HEADS * VD, D), (2 * HEADS * VD) ** -0.5, 0.1875, ((0, 4),)),
        "out_b": scatter_about(streams_of[10], (HEADS * VD, D), (2 * HEADS * VD) ** -0.5, 0.1875, ((0, 4),)),
        "norm_gain": jnp.clip(1.0 + 0.18 * jax.random.normal(streams_of[11], (D,), jnp.float32), 0.1, 1.9),
        "w_gate": scatter_about(streams_of[12], (D, FF), D ** -0.5, 0.125, ((0, 8), (1, 4))),
        "w_up": scatter_about(streams_of[13], (D, FF), D ** -0.5, 0.125, ((0, 8), (1, 4))),
        "w_down": scatter_about(streams_of[14], (FF, D), (FF // 8) ** -0.5, 0.21875, ((0, 4), (1, 8))),
    }


eps_norm = 1e-06
head_scale = 0.8

def group_attend(queries, keys, values, lambdas, gain, width):
    total = queries.shape[0]
    heads = lambdas.shape[0]
    block = math.gcd(total, 512)
    query_blocks = queries.reshape(total // block, block, heads, 2, width)
    key_rows = keys.reshape(total, heads, 2, width).astype(jnp.float32)
    value_rows = values.reshape(total, heads, values.shape[1] // heads).astype(jnp.float32)

    def one_block(query_block):
        scores = jnp.einsum('qhme,khme->mhqk', query_block.astype(jnp.float32), key_rows) * width ** (-0.5)
        peak = lax.optimization_barrier(jnp.max(scores, axis=-1, keepdims=True))
        weights = jnp.exp(scores - peak)
        denom = lax.optimization_barrier(jnp.sum(weights, axis=-1))
        rounded = lax.optimization_barrier(weights.astype(jnp.bfloat16)).astype(jnp.float32)
        numer = jnp.einsum('mhqk,khv->mhqv', rounded, value_rows)
        ratio = numer / denom[..., None]
        mixed = ratio[0] - lambdas[:, None, None] * ratio[1]
        inverse = lax.rsqrt(lax.optimization_barrier(jnp.mean(mixed * mixed, axis=-1, keepdims=True)) + eps_norm)
        normed = mixed * inverse * gain * head_scale
        return jnp.transpose(normed, (1, 0, 2)).reshape(block, -1).astype(jnp.bfloat16)
    return lax.map(one_block, query_blocks).reshape(total, -1)

def reference(residual, queries_a, keys_a, values_a, queries_b, keys_b, values_b, mix_lambda, head_gain, out_a, out_b, norm_gain, w_gate, w_up, w_down):
    heads_a = group_attend(queries_a, keys_a, values_a, mix_lambda[0], head_gain[0], QA)
    heads_b = group_attend(queries_b, keys_b, values_b, mix_lambda[1], head_gain[1], QB)
    total = residual.shape[0]
    block = math.gcd(total, 2048)
    count = total // block

    def row_block(inputs):
        residual_rows, first_rows, second_rows = inputs
        mixed = jnp.dot(first_rows, out_a, preferred_element_type=jnp.float32)
        mixed = mixed + jnp.dot(second_rows, out_b, preferred_element_type=jnp.float32)
        summed = residual_rows.astype(jnp.float32) + mixed
        inverse = lax.rsqrt(lax.optimization_barrier(jnp.mean(summed * summed, axis=-1, keepdims=True)) + eps_norm)
        normed = (summed * inverse * norm_gain).astype(jnp.bfloat16)
        gate = jnp.dot(normed, w_gate, preferred_element_type=jnp.float32)
        upward = jnp.dot(normed, w_up, preferred_element_type=jnp.float32)
        hidden = (jax.nn.silu(gate) * upward).astype(jnp.bfloat16)
        channel = jnp.dot(hidden, w_down, preferred_element_type=jnp.float32)
        return (summed + 0.5 * channel).astype(jnp.bfloat16)
    result = lax.map(row_block, (residual.reshape(count, block, -1), heads_a.reshape(count, block, -1), heads_b.reshape(count, block, -1)))
    return result.reshape(total, -1)
```

```python
import functools
import math

import jax
import jax.numpy as jnp
from jax import lax
from jax.experimental import pallas as pl
from jax.experimental.pallas import tpu as pltpu
from jax.sharding import PartitionSpec as P

eps_norm = 1e-06
head_scale = 0.8
MESH = pl.DeviceIdType.MESH
CHUNKS = 2
NT = (((1,), (1,)), ((), ()))


def ring_to_sp(pos, n):
    late = pos // (n // 2)
    return (1 - late) * 2 * pos + late * (2 * (n - 1 - pos) + 1)


def sp_to_ring(index, n):
    odd = index % 2
    return (1 - odd) * (index // 2) + odd * (n - 1 - (index - odd) // 2)


def kernel(
    n, tp, residual, qa, ka, va, qb, kb, vb, lam, gain, oa, ob, ngain, wg, wu, wd, out,
    kv_all, wg_all, wu_all, wd_all, out_all, heads_all, summed, normed, hidden, channel, sbuf, rbuf,
    mine, local_sem, ring_send, ring_recv, out_send, out_recv, head_send, head_recv, red_send, red_recv,
):
    rows, width = residual.shape
    heads = lam.shape[1]
    sa, sb = qa.shape[1] // (2 * heads), qb.shape[1] // (2 * heads)
    vd = va.shape[1] // heads
    hv = heads * vd
    block = math.gcd(rows, 128)
    nb = rows // block
    share = width // tp
    sp_me, tp_me = lax.axis_index("sp"), lax.axis_index("tp")
    pos = sp_to_ring(sp_me, n)
    targets = (ring_to_sp((pos + 1) % n, n), ring_to_sp((pos + n - 1) % n, n))
    peers = [(tp_me + k) % tp for k in range(1, tp)]

    ck, cv = ka.shape[1], ka.shape[1] + kb.shape[1]
    own_kv = kv_all.at[sp_me]
    own = [
        (ka, own_kv.at[:, pl.ds(0, ck)]),
        (kb, own_kv.at[:, pl.ds(ck, kb.shape[1])]),
        (va, own_kv.at[:, pl.ds(cv, hv)]),
        (vb, own_kv.at[:, pl.ds(cv + hv, hv)]),
        (wg, wg_all.at[sp_me]),
        (wu, wu_all.at[sp_me]),
        (wd, wd_all.at[sp_me]),
        (oa, out_all.at[tp_me, pl.ds(0, hv)]),
        (ob, out_all.at[tp_me, pl.ds(hv, hv)]),
    ]
    copies = [pltpu.make_async_copy(s, d, local_sem.at[i]) for i, (s, d) in enumerate(own)]
    for c in copies:
        c.start()

    barrier = pltpu.get_barrier_semaphore()
    for target in targets:
        pl.semaphore_signal(barrier, inc=1, device_id={"sp": target}, device_id_type=MESH)
    for peer in peers:
        pl.semaphore_signal(barrier, inc=1, device_id={"tp": peer}, device_id_type=MESH)
    for c in copies:
        c.wait()
    pl.semaphore_wait(barrier, 2 + len(peers))

    gathered = (kv_all, wg_all, wu_all, wd_all)

    def piece(a, c, d, t, dist):
        ref = gathered[a]
        owner = ring_to_sp((pos + n - dist) % n if d == 0 else (pos + dist) % n, n)
        part = ref.shape[1] // (2 * CHUNKS)
        view = ref.at[owner, pl.ds((d * CHUNKS + c) * part, part)]
        return pltpu.make_async_remote_copy(
            src_ref=view,
            dst_ref=view,
            send_sem=ring_send.at[a, c, d, t],
            recv_sem=ring_recv.at[a, c, d, t],
            device_id={"sp": targets[d]},
            device_id_type=MESH,
        )

    def begin(a):
        for c in range(CHUNKS):
            for d in range(2):
                piece(a, c, d, 0, 0).start()

    def step(a, c, t):
        for d in range(2):
            piece(a, c, d, t, t + 1).wait_recv()

            @pl.when(t + 1 < n - 1)
            def _():
                piece(a, c, d, t + 1, t + 1).start()

    def phase(a, work):
        def body(t, _):
            for c in range(CHUNKS):
                step(a, c, t)
                work(t * CHUNKS + c)
            return 0

        lax.fori_loop(0, n - 1, body, 0)

    slots = CHUNKS * (n - 1)

    begin(0)
    begin(1)

    def out_copy(k, target, slot):
        return pltpu.make_async_remote_copy(
            src_ref=out_all.at[slot], dst_ref=out_all.at[slot],
            send_sem=out_send.at[k], recv_sem=out_recv.at[k],
            device_id={"tp": target}, device_id_type=MESH,
        )

    def head_copy(k, target, slot):
        return pltpu.make_async_remote_copy(
            src_ref=mine, dst_ref=heads_all.at[slot],
            send_sem=head_send.at[k], recv_sem=head_recv.at[k],
            device_id={"tp": target}, device_id_type=MESH,
        )

    for k, peer in enumerate(peers):
        out_copy(k, peer, tp_me).start()

    phase(0, lambda slot: None)
    begin(2)

    total = n * rows

    def attend(group, r):
        queries = qa if group == 0 else qb
        size = sa if group == 0 else sb
        base = 0 if group == 0 else ck
        factor = size ** (-0.5) * math.log2(math.e)
        at = pl.ds(pl.multiple_of(r * block, block), block)
        for h in range(heads):
            start = 2 * h * size
            query = queries[at, start : start + 2 * size]
            value = kv_all[:, :, cv + group * hv + h * vd : cv + group * hv + (h + 1) * vd].reshape(total, vd)
            lanes = lax.broadcasted_iota(jnp.int32, query.shape, 1)
            ratios = []
            for j in range(2):
                if size % 128 == 0:
                    q = query[:, j * size : (j + 1) * size]
                    low = base + start + j * size
                    key = kv_all[:, :, low : low + size].reshape(total, size)
                else:
                    q = jnp.where(lanes // size == j, query, jnp.zeros_like(query))
                    low = base + start
                    key = kv_all[:, :, low : low + 2 * size].reshape(total, 2 * size)
                scores = lax.dot_general(q, key, NT, preferred_element_type=jnp.float32)
                peak = jnp.max(scores, axis=1, keepdims=True)
                weights = jnp.exp2((scores - peak) * factor)
                denom = jnp.sum(weights, axis=1, keepdims=True)
                numer = jnp.dot(weights.astype(jnp.bfloat16), value, preferred_element_type=jnp.float32)
                ratios.append(numer / denom)
            mixed = ratios[0] - lam[group, h] * ratios[1]
            inverse = lax.rsqrt(jnp.mean(mixed * mixed, axis=-1, keepdims=True) + eps_norm)
            result = mixed * inverse * gain[group : group + 1, :] * head_scale
            col = group * hv + h * vd
            mine[at, col : col + vd] = result.astype(jnp.bfloat16)

    def attend_slot(slot):
        @pl.when(slot < nb)
        def _():
            attend(0, slot)

        @pl.when((slot >= nb) & (slot < 2 * nb))
        def _():
            attend(1, slot - nb)

    phase(1, attend_slot)
    for slot in range(slots, 2 * nb):
        attend_slot(slot)
    begin(3)
    for k, peer in enumerate(peers):
        head_copy(k, peer, tp_me).start()

    def arrived():
        for k in range(tp - 1):
            source = (tp_me + tp - 1 - k) % tp
            head_copy(k, peers[k], source).wait_recv()
            out_copy(k, peers[k], source).wait_recv()
        heads_all[tp_me] = mine[...]

    def project(r):
        at = pl.ds(pl.multiple_of(r * block, block), block)
        acc = residual[at, :].astype(jnp.float32)
        for d in range(tp):
            acc = acc + jnp.dot(heads_all[d, at, :], out_all[d], preferred_element_type=jnp.float32)
        inverse = lax.rsqrt(jnp.mean(acc * acc, axis=-1, keepdims=True) + eps_norm)
        normed[at, :] = (acc * inverse * ngain[...]).astype(jnp.bfloat16)
        summed[at, :] = acc

    late = slots - nb

    def project_slot(slot):
        @pl.when(slot == late)
        def _():
            arrived()

        @pl.when(slot >= late)
        def _():
            project(slot - late)

    phase(2, project_slot)

    units = wg_all.shape[2]
    tile = math.gcd(units, 128)
    tiles = units // tile

    def feed(i):
        at = pl.ds(pl.multiple_of(i * tile, tile), tile)
        x = normed[...]
        gate = jnp.dot(x, wg_all[:, :, at].reshape(width, tile), preferred_element_type=jnp.float32)
        upward = jnp.dot(x, wu_all[:, :, at].reshape(width, tile), preferred_element_type=jnp.float32)
        hidden[:, at] = (gate / (1.0 + jnp.exp(-gate)) * upward).astype(jnp.bfloat16)

    per = -(-tiles // slots)

    def feed_slot(slot):
        for k in range(per):
            @pl.when(slot * per + k < tiles)
            def _():
                feed(slot * per + k)

    phase(3, feed_slot)

    cols = wd_all.shape[2]
    ratio = share // cols
    for d in range(tp):
        for s in range(ratio):
            channel[d, :, s * cols : (s + 1) * cols] = jnp.dot(
                hidden[...], wd_all[d * ratio + s], preferred_element_type=jnp.float32
            )

    bit, used, pending = 1, 0, []
    while bit < tp:
        flag = (tp_me // bit) % 2
        partner = tp_me + bit - 2 * bit * flag
        count = tp // (2 * bit)
        batch = []
        for m in range(count):
            give = tp_me % bit + bit * (1 - flag) + 2 * bit * m
            keep = tp_me % bit + bit * flag + 2 * bit * m
            sbuf[give] = channel[give].astype(jnp.bfloat16)
            copy = pltpu.make_async_remote_copy(
                src_ref=sbuf.at[give], dst_ref=rbuf.at[used],
                send_sem=red_send.at[used], recv_sem=red_recv.at[used],
                device_id={"tp": partner}, device_id_type=MESH,
            )
            copy.start()
            batch.append((copy, keep, used))
            used += 1
        for copy, keep, slot in batch:
            copy.wait_recv()
            channel[keep] = channel[keep] + rbuf[slot].astype(jnp.float32)
            pending.append(copy)
        bit *= 2

    at = pl.ds(pl.multiple_of(tp_me * share, share), share)
    out[...] = (summed[:, at] + 0.5 * channel[tp_me]).astype(jnp.bfloat16)

    for copy in pending:
        copy.wait_send()
    for k, peer in enumerate(peers):
        out_copy(k, peer, tp_me).wait_send()
        head_copy(k, peer, tp_me).wait_send()

    def drain(t, _):
        for a in range(len(gathered)):
            for c in range(CHUNKS):
                for d in range(2):
                    piece(a, c, d, t, t).wait_send()
        return 0

    lax.fori_loop(0, n - 1, drain, 0)


def local(
    n, tp, residual, queries_a, keys_a, values_a, queries_b, keys_b, values_b, mix_lambda, head_gain,
    out_a, out_b, norm_gain, w_gate, w_up, w_down,
):
    rows, width = residual.shape
    share = width // tp
    units = w_gate.shape[1]
    hv = out_a.shape[0]
    span = keys_a.shape[1] + keys_b.shape[1] + values_a.shape[1] + values_b.shape[1]
    vmem, anywhere = pl.BlockSpec(memory_space=pltpu.VMEM), pl.BlockSpec(memory_space=pl.ANY)
    smem = pl.BlockSpec(memory_space=pltpu.SMEM)
    bf16, f32 = jnp.bfloat16, jnp.float32
    dma = pltpu.SemaphoreType.DMA
    return pl.pallas_call(
        functools.partial(kernel, n, tp),
        out_shape=jax.ShapeDtypeStruct((rows, share), bf16),
        in_specs=[
            vmem, vmem, anywhere, anywhere, vmem, anywhere, anywhere, smem, vmem,
            anywhere, anywhere, vmem, anywhere, anywhere, anywhere,
        ],
        out_specs=vmem,
        scratch_shapes=[
            pltpu.VMEM((n, rows, span), bf16),
            pltpu.VMEM((n,) + w_gate.shape, bf16),
            pltpu.VMEM((n,) + w_up.shape, bf16),
            pltpu.VMEM((n,) + w_down.shape, bf16),
            pltpu.VMEM((tp, 2 * hv, width), bf16),
            pltpu.VMEM((tp, rows, 2 * hv), bf16),
            pltpu.VMEM((rows, width), f32),
            pltpu.VMEM((rows, width), bf16),
            pltpu.VMEM((rows, units), bf16),
            pltpu.VMEM((tp, rows, share), f32),
            pltpu.VMEM((tp, rows, share), bf16),
            pltpu.VMEM((tp - 1, rows, share), bf16),
            pltpu.VMEM((rows, 2 * hv), bf16),
            dma((9,)),
            dma((4, CHUNKS, 2, n - 1)),
            dma((4, CHUNKS, 2, n - 1)),
            dma((tp - 1,)),
            dma((tp - 1,)),
            dma((tp - 1,)),
            dma((tp - 1,)),
            dma((tp - 1,)),
            dma((tp - 1,)),
        ],
        compiler_params=pltpu.CompilerParams(
            collective_id=0, has_side_effects=True, vmem_limit_bytes=63 * 1024 * 1024
        ),
        name="layer",
    )(
        residual, queries_a, keys_a, values_a, queries_b, keys_b, values_b, mix_lambda, head_gain,
        out_a, out_b, norm_gain.reshape(1, -1), w_gate, w_up, w_down,
    )


def solution(mesh):
    in_specs = (
        P("sp", None),
        P("sp", "tp"),
        P("sp", "tp"),
        P("sp", "tp"),
        P("sp", "tp"),
        P("sp", "tp"),
        P("sp", "tp"),
        P(None, "tp"),
        P(),
        P("tp", None),
        P("tp", None),
        P(),
        P("sp", "tp"),
        P("sp", "tp"),
        P("tp", "sp"),
    )
    body = functools.partial(local, mesh.shape["sp"], mesh.shape["tp"])
    return jax.shard_map(body, mesh=mesh, in_specs=in_specs, out_specs=P("sp", "tp"), check_vma=False)
```

```python
import functools
import math

import jax
import jax.numpy as jnp
from jax import lax
from jax.experimental import pallas as pl
from jax.experimental.pallas import tpu as pltpu
from jax.sharding import PartitionSpec as P

eps_norm = 1e-06
head_scale = 0.8
MESH = pl.DeviceIdType.MESH
CHUNKS = 2
CUTS = 3
NT = (((1,), (1,)), ((), ()))


def ring_to_sp(pos, n):
    late = pos // (n // 2)
    return (1 - late) * 2 * pos + late * (2 * (n - 1 - pos) + 1)


def sp_to_ring(index, n):
    odd = index % 2
    return (1 - odd) * (index // 2) + odd * (n - 1 - (index - odd) // 2)


def flip(index, bit):
    return index + bit - 2 * bit * ((index // bit) % 2)


def flip_all(index, mask):
    bit = 1
    while bit <= mask:
        if mask & bit:
            index = flip(index, bit)
        bit *= 2
    return index


def kernel(
    n, tp, residual, qa, ka, va, qb, kb, vb, lam, gain, oa, ob, ngain, wg, wu, wd, out,
    kv_all, wg_turn, wu_turn, wg_all, wu_all, wd_all, out_all, heads_all, summed, normed, hidden, channel, sbuf,
    rbuf, tbuf, mine, local_sem, ring_send, ring_recv, cube_send, cube_recv, out_send, out_recv, head_send,
    head_recv, norm_send, norm_recv, red_send, red_recv,
):
    rows, width = residual.shape
    heads = lam.shape[1]
    sa, sb = qa.shape[1] // (2 * heads), qb.shape[1] // (2 * heads)
    vd = va.shape[1] // heads
    hv = heads * vd
    total = n * rows
    block = math.gcd(rows, 1 << min(7, ((1 << 19) // total).bit_length() - 1))
    nb = rows // block
    share = width // tp
    depth, units = wg.shape
    half = units // 2
    sp_me, tp_me = lax.axis_index("sp"), lax.axis_index("tp")
    pos = sp_to_ring(sp_me, n)
    targets = (ring_to_sp((pos + 1) % n, n), ring_to_sp((pos + n - 1) % n, n))
    peers = [(tp_me + k) % tp for k in range(1, tp)]
    pair = n // 4
    side = (sp_me // pair) % 2
    mate = flip(sp_me, pair)
    bits = [pair, n // 2]
    while bits[-1 if len(bits) > 2 else 0] > 1:
        bits.append(bits[-1] // 2 if len(bits) > 2 else pair // 2)

    ck, cv = ka.shape[1], ka.shape[1] + kb.shape[1]
    own_kv = kv_all.at[sp_me]
    own = [
        (ka, own_kv.at[:, pl.ds(0, ck)]),
        (kb, own_kv.at[:, pl.ds(ck, kb.shape[1])]),
        (va, own_kv.at[:, pl.ds(cv, hv)]),
        (vb, own_kv.at[:, pl.ds(cv + hv, hv)]),
        (wd.at[pl.ds(pl.multiple_of(side * half, half), half)], wd_all.at[sp_me]),
        (oa, out_all.at[tp_me, pl.ds(0, hv)]),
        (ob, out_all.at[tp_me, pl.ds(hv, hv)]),
    ]
    copies = [pltpu.make_async_copy(s, d, local_sem.at[i]) for i, (s, d) in enumerate(own)]
    for c in copies:
        c.start()

    barrier = pltpu.get_barrier_semaphore()
    for target in list(targets) + [flip(sp_me, bit) for bit in bits]:
        pl.semaphore_signal(barrier, inc=1, device_id={"sp": target}, device_id_type=MESH)
    for peer in peers:
        pl.semaphore_signal(barrier, inc=1, device_id={"tp": peer}, device_id_type=MESH)
    for c in copies:
        c.wait()
    pl.semaphore_wait(barrier, 2 + len(bits) + len(peers))

    def piece(c, d, t, dist):
        owner = ring_to_sp((pos + n - dist) % n if d == 0 else (pos + dist) % n, n)
        part = rows // (2 * CHUNKS)
        view = kv_all.at[owner, pl.ds((d * CHUNKS + c) * part, part)]
        return pltpu.make_async_remote_copy(
            src_ref=view, dst_ref=view,
            send_sem=ring_send.at[c, d, t], recv_sem=ring_recv.at[c, d, t],
            device_id={"sp": targets[d]}, device_id_type=MESH,
        )

    for c in range(CHUNKS):
        for d in range(2):
            piece(c, d, 0, 0).start()

    def out_copy(k, target, slot):
        return pltpu.make_async_remote_copy(
            src_ref=out_all.at[slot], dst_ref=out_all.at[slot],
            send_sem=out_send.at[k], recv_sem=out_recv.at[k],
            device_id={"tp": target}, device_id_type=MESH,
        )

    def head_copy(k, target, slot):
        return pltpu.make_async_remote_copy(
            src_ref=mine, dst_ref=heads_all.at[slot],
            send_sem=head_send.at[k], recv_sem=head_recv.at[k],
            device_id={"tp": target}, device_id_type=MESH,
        )

    for k, peer in enumerate(peers):
        out_copy(k, peer, tp_me).start()

    tile = math.gcd(units, 128)

    def turn(i):
        at = pl.ds(pl.multiple_of(i * tile, tile), tile)
        wg_turn[at, :] = wg[:, at].T
        wu_turn[at, :] = wu[:, at].T

    turns = units // tile
    per = -(-turns // (n - 1))

    def circulate(t, _):
        for c in range(CHUNKS):
            for d in range(2):
                piece(c, d, t, t + 1).wait_recv()

                @pl.when(t + 1 < n - 1)
                def _():
                    piece(c, d, t + 1, t + 1).start()

        for k in range(per):
            @pl.when(t * per + k < turns)
            def _():
                turn(t * per + k)

        return 0

    lax.fori_loop(0, n - 1, circulate, 0)
    wg_all[sp_me] = wg_turn[pl.ds(pl.multiple_of(side * half, half), half), :]
    wu_all[sp_me] = wu_turn[pl.ds(pl.multiple_of(side * half, half), half), :]

    gathered = (wg_all, wu_all, wd_all)
    whole = (wg_turn, wu_turn, wd)

    def cube(a, held, k, arriving):
        mask = held | bits[k]
        owner = flip_all(sp_me, mask if arriving else held)
        dst = gathered[a].at[owner]
        src = dst
        if k == 0 and not arriving:
            src = whole[a].at[pl.ds(pl.multiple_of((1 - side) * half, half), half)]
        return pltpu.make_async_remote_copy(
            src_ref=src, dst_ref=dst,
            send_sem=cube_send.at[a, mask], recv_sem=cube_recv.at[a, mask],
            device_id={"sp": flip(sp_me, bits[k])}, device_id_type=MESH,
        )

    order = [0]
    came = {}
    for k, bit in enumerate(bits):
        for held in list(order):
            came[held | bit] = (held, k)
            order.append(held | bit)

    def forward(a, mask):
        first = came[mask][1] + 1 if mask else 0
        for k in range(first, len(bits)):
            cube(a, mask, k, False).start()

    def arrive(a, mask):
        held, k = came[mask]
        cube(a, held, k, True).wait_recv()
        forward(a, mask)

    for a in range(3):
        forward(a, 0)
    events = []
    for k in range(len(bits)):
        for a in range(3):
            for mask in order[1:]:
                if came[mask][1] == k:
                    events.append((a, mask))

    def take(count):
        for a, mask in events[:count]:
            arrive(a, mask)
        del events[:count]

    def attend(group, r):
        queries = qa if group == 0 else qb
        size = sa if group == 0 else sb
        base = 0 if group == 0 else ck
        factor = size ** (-0.5) * math.log2(math.e)
        at = pl.ds(pl.multiple_of(r * block, block), block)
        for h in range(heads):
            start = 2 * h * size
            query = queries[at, start : start + 2 * size]
            value = kv_all[:, :, cv + group * hv + h * vd : cv + group * hv + (h + 1) * vd].reshape(total, vd)
            lanes = lax.broadcasted_iota(jnp.int32, query.shape, 1)
            ratios = []
            for j in range(2):
                if size % 128 == 0:
                    q = query[:, j * size : (j + 1) * size]
                    low = base + start + j * size
                    key = kv_all[:, :, low : low + size].reshape(total, size)
                else:
                    q = jnp.where(lanes // size == j, query, jnp.zeros_like(query))
                    low = base + start
                    key = kv_all[:, :, low : low + 2 * size].reshape(total, 2 * size)
                scores = lax.dot_general(q, key, NT, preferred_element_type=jnp.float32)
                peak = jnp.max(scores, axis=1, keepdims=True)
                weights = jnp.exp2((scores - peak) * factor)
                denom = jnp.sum(weights, axis=1, keepdims=True)
                numer = jnp.dot(weights.astype(jnp.bfloat16), value, preferred_element_type=jnp.float32)
                ratios.append(numer / denom)
            mixed = ratios[0] - lam[group, h] * ratios[1]
            inverse = lax.rsqrt(jnp.mean(mixed * mixed, axis=-1, keepdims=True) + eps_norm)
            result = mixed * inverse * gain[group : group + 1, :] * head_scale
            col = group * hv + h * vd
            mine[at, col : col + vd] = result.astype(jnp.bfloat16)

    early = sum(1 for _, mask in events if came[mask][1] < 2)
    portion = -(-early // (2 * CUTS))
    cuts = [nb * i // CUTS for i in range(CUTS + 1)]
    for group in range(2):
        for i in range(CUTS):
            def body(r, _, group=group):
                attend(group, r)
                return 0

            lax.fori_loop(cuts[i], cuts[i + 1], body, 0)
            take(min(portion, early))
            early -= min(portion, early)

    for k, peer in enumerate(peers):
        head_copy(k, peer, tp_me).start()
    for k in range(tp - 1):
        source = (tp_me + tp - 1 - k) % tp
        head_copy(k, peers[k], source).wait_recv()
        out_copy(k, peers[k], source).wait_recv()
    heads_all[tp_me] = mine[...]

    def project(r, _):
        at = pl.ds(pl.multiple_of(r * block, block), block)
        acc = residual[at, :].astype(jnp.float32)
        for d in range(tp):
            acc = acc + jnp.dot(heads_all[d, at, :], out_all[d], preferred_element_type=jnp.float32)
        inverse = lax.rsqrt(jnp.mean(acc * acc, axis=-1, keepdims=True) + eps_norm)
        scaled = (acc * inverse * ngain[...]).astype(jnp.bfloat16)
        for d in range(tp):
            normed[side, d, at, :] = scaled[:, d * share : (d + 1) * share]
            summed[d, at, :] = acc[:, d * share : (d + 1) * share].astype(summed.dtype)
        return 0

    lax.fori_loop(0, nb, project, 0)

    def swap(arriving):
        there = 1 - side if arriving else side
        view = normed.at[there, tp_me]
        return pltpu.make_async_remote_copy(
            src_ref=view, dst_ref=view, send_sem=norm_send.at[0], recv_sem=norm_recv.at[0],
            device_id={"sp": mate}, device_id_type=MESH,
        )

    def spread(k, target, slot):
        view = normed.at[1 - side, slot]
        return pltpu.make_async_remote_copy(
            src_ref=view, dst_ref=view, send_sem=norm_send.at[1 + k], recv_sem=norm_recv.at[1 + k],
            device_id={"tp": target}, device_id_type=MESH,
        )

    swap(False).start()
    take(sum(1 for a, _ in events if a == 0))
    swap(True).wait_recv()
    for k, peer in enumerate(peers):
        spread(k, peer, tp_me).start()
    take(sum(1 for a, _ in events if a == 1))

    step_cols = share // depth

    def feed(where):
        gate = jnp.zeros((rows, half), jnp.float32)
        upward = jnp.zeros((rows, half), jnp.float32)
        for s in range(n):
            low = (s % step_cols) * depth
            x = normed[where, s // step_cols, :, low : low + depth]
            gate = gate + lax.dot_general(x, wg_all[s], NT, preferred_element_type=jnp.float32)
            upward = upward + lax.dot_general(x, wu_all[s], NT, preferred_element_type=jnp.float32)
        hidden[where] = (gate / (1.0 + jnp.exp(-gate)) * upward).astype(jnp.bfloat16)

    def feed_one(i, _):
        @pl.when(i == 1)
        def _():
            for k in range(tp - 1):
                spread(k, peers[k], (tp_me + tp - 1 - k) % tp).wait_recv()

        feed((side + i) % 2)
        return 0

    lax.fori_loop(0, 2, feed_one, 0)
    take(len(events))

    cols = wd_all.shape[2]
    ratio = share // cols
    low_bit = tp_me % 2

    def block_sum(d, where):
        return [
            jnp.dot(hidden[where], wd_all[d * ratio + s], preferred_element_type=jnp.float32)
            for s in range(ratio)
        ]

    used, pending = 0, []

    def send(src, **target):
        nonlocal used
        copy = pltpu.make_async_remote_copy(
            src_ref=src, dst_ref=rbuf.at[used], send_sem=red_send.at[used], recv_sem=red_recv.at[used],
            device_id=target, device_id_type=MESH,
        )
        copy.start()
        pending.append(copy)
        used += 1

    for i in range(2):
        for m in range(tp // 2):
            d = 2 * m + (1 - low_bit if i == 0 else low_bit)
            for where in range(2):
                for s, value in enumerate(block_sum(d, where)):
                    if i == 0:
                        sbuf[2 * m + where, :, s * cols : (s + 1) * cols] = value.astype(jnp.bfloat16)
                    else:
                        channel[2 * m + where, :, s * cols : (s + 1) * cols] = value
                if i == 0:
                    send(sbuf.at[2 * m + where], tp=flip(tp_me, 1))
    for m in range(tp):
        pending[m].wait_recv()
        channel[m] = channel[m] + rbuf[m].astype(jnp.float32)

    bit, sent = 2, 0
    while bit < tp:
        flag = (tp_me // bit) % 2
        count = tp // (2 * bit)
        batch = []
        for m in range(count):
            give = (tp_me % bit + bit * (1 - flag) + 2 * bit * m) // 2
            keep = (tp_me % bit + bit * flag + 2 * bit * m) // 2
            for i in range(2):
                where = (1 - side) if i == 0 else side
                tbuf[sent] = channel[2 * give + where].astype(jnp.bfloat16)
                batch.append((used, 2 * keep + where))
                send(tbuf.at[sent], tp=flip(tp_me, bit))
                sent += 1
        for slot, keep in batch:
            pending[slot].wait_recv()
            channel[keep] = channel[keep] + rbuf[slot].astype(jnp.float32)
        bit *= 2
    tbuf[sent] = channel[2 * (tp_me // 2) + 1 - side].astype(jnp.bfloat16)
    last = used
    send(tbuf.at[sent], sp=mate)
    pending[last].wait_recv()
    final = channel[2 * (tp_me // 2) + side] + rbuf[last].astype(jnp.float32)
    out[...] = (summed[tp_me] + 0.5 * final).astype(jnp.bfloat16)

    for copy in pending:
        copy.wait_send()
    swap(False).wait_send()
    for k, peer in enumerate(peers):
        out_copy(k, peer, tp_me).wait_send()
        head_copy(k, peer, tp_me).wait_send()
        spread(k, peer, tp_me).wait_send()
    for a in range(3):
        for mask in order[1:]:
            held, k = came[mask]
            cube(a, held, k, False).wait_send()

    def drain(t, _):
        for c in range(CHUNKS):
            for d in range(2):
                piece(c, d, t, t).wait_send()
        return 0

    lax.fori_loop(0, n - 1, drain, 0)


def local(
    n, tp, residual, queries_a, keys_a, values_a, queries_b, keys_b, values_b, mix_lambda, head_gain,
    out_a, out_b, norm_gain, w_gate, w_up, w_down,
):
    rows, width = residual.shape
    share = width // tp
    units = w_gate.shape[1]
    hv = out_a.shape[0]
    span = keys_a.shape[1] + keys_b.shape[1] + values_a.shape[1] + values_b.shape[1]
    vmem, anywhere = pl.BlockSpec(memory_space=pltpu.VMEM), pl.BlockSpec(memory_space=pl.ANY)
    smem = pl.BlockSpec(memory_space=pltpu.SMEM)
    bf16, f32 = jnp.bfloat16, jnp.float32
    dma = pltpu.SemaphoreType.DMA
    return pl.pallas_call(
        functools.partial(kernel, n, tp),
        out_shape=jax.ShapeDtypeStruct((rows, share), bf16),
        in_specs=[
            vmem, vmem, anywhere, anywhere, vmem, anywhere, anywhere, smem, vmem,
            anywhere, anywhere, vmem, vmem, vmem, anywhere,
        ],
        out_specs=vmem,
        scratch_shapes=[
            pltpu.VMEM((n, rows, span), bf16),
            pltpu.VMEM((units, w_gate.shape[0]), bf16),
            pltpu.VMEM((units, w_gate.shape[0]), bf16),
            pltpu.VMEM((n, units // 2, w_gate.shape[0]), bf16),
            pltpu.VMEM((n, units // 2, w_gate.shape[0]), bf16),
            pltpu.VMEM((n, units // 2, w_down.shape[1]), bf16),
            pltpu.VMEM((tp, 2 * hv, width), bf16),
            pltpu.VMEM((tp, rows, 2 * hv), bf16),
            pltpu.VMEM((tp, rows, share), f32),
            pltpu.VMEM((2, tp, rows, share), bf16),
            pltpu.VMEM((2, rows, units // 2), bf16),
            pltpu.VMEM((tp, rows, share), f32),
            pltpu.VMEM((tp, rows, share), bf16),
            pltpu.VMEM((2 * tp - 1, rows, share), bf16),
            pltpu.VMEM((tp - 1, rows, share), bf16),
            pltpu.VMEM((rows, 2 * hv), bf16),
            dma((7,)),
            dma((CHUNKS, 2, n - 1)),
            dma((CHUNKS, 2, n - 1)),
            dma((3, n)),
            dma((3, n)),
            dma((tp - 1,)),
            dma((tp - 1,)),
            dma((tp - 1,)),
            dma((tp - 1,)),
            dma((tp,)),
            dma((tp,)),
            dma((2 * tp - 1,)),
            dma((2 * tp - 1,)),
        ],
        compiler_params=pltpu.CompilerParams(
            collective_id=0, has_side_effects=True, vmem_limit_bytes=63 * 1024 * 1024
        ),
        name="layer",
    )(
        residual, queries_a, keys_a, values_a, queries_b, keys_b, values_b, mix_lambda, head_gain,
        out_a, out_b, norm_gain.reshape(1, -1), w_gate, w_up, w_down,
    )


def solution(mesh):
    in_specs = (
        P("sp", None),
        P("sp", "tp"),
        P("sp", "tp"),
        P("sp", "tp"),
        P("sp", "tp"),
        P("sp", "tp"),
        P("sp", "tp"),
        P(None, "tp"),
        P(),
        P("tp", None),
        P("tp", None),
        P(),
        P("sp", "tp"),
        P("sp", "tp"),
        P("tp", "sp"),
    )
    body = functools.partial(local, mesh.shape["sp"], mesh.shape["tp"])
    return jax.shard_map(body, mesh=mesh, in_specs=in_specs, out_specs=P("sp", "tp"), check_vma=False)
```

```python
import functools
import math

import jax
import jax.numpy as jnp
from jax import lax
from jax.experimental import pallas as pl
from jax.experimental.pallas import tpu as pltpu
from jax.sharding import PartitionSpec as P

eps_norm = 1e-06
head_scale = 0.8
MESH = pl.DeviceIdType.MESH
CHUNKS = 2
CUTS = 3
NT = (((1,), (1,)), ((), ()))


def ring_to_sp(pos, n):
    late = pos // (n // 2)
    return (1 - late) * 2 * pos + late * (2 * (n - 1 - pos) + 1)


def sp_to_ring(index, n):
    odd = index % 2
    return (1 - odd) * (index // 2) + odd * (n - 1 - (index - odd) // 2)


def flip(index, bit):
    return index + bit - 2 * bit * ((index // bit) % 2)


def flip_all(index, mask):
    bit = 1
    while bit <= mask:
        if mask & bit:
            index = flip(index, bit)
        bit *= 2
    return index


def kernel(
    n, tp, residual, qa, ka, va, qb, kb, vb, lam, gain, oa, ob, ngain, wg, wu, wd, out,
    kv_all, wg_turn, wu_turn, wg_all, wu_all, wd_all, out_all, heads_all, summed, normed, hidden, channel, sbuf,
    rbuf, tbuf, ubuf, mine, local_sem, ring_send, ring_recv, cube_send, cube_recv, out_send, out_recv, head_send,
    head_recv, swap_sem, norm_send, norm_recv, red_send, red_recv,
):
    rows, width = residual.shape
    heads = lam.shape[1]
    sa, sb = qa.shape[1] // (2 * heads), qb.shape[1] // (2 * heads)
    vd = va.shape[1] // heads
    hv = heads * vd
    total = n * rows
    block = math.gcd(rows, 1 << min(7, ((1 << 19) // total).bit_length() - 1))
    nb = rows // block
    share = width // tp
    depth, units = wg.shape
    half = units // 2
    sp_me, tp_me = lax.axis_index("sp"), lax.axis_index("tp")
    pos = sp_to_ring(sp_me, n)
    targets = (ring_to_sp((pos + 1) % n, n), ring_to_sp((pos + n - 1) % n, n))
    peers = [(tp_me + k) % tp for k in range(1, tp)]
    pair = n // 4
    side = (sp_me // pair) % 2
    mate = flip(sp_me, pair)
    bits = [pair, n // 2]
    while bits[-1 if len(bits) > 2 else 0] > 1:
        bits.append(bits[-1] // 2 if len(bits) > 2 else pair // 2)

    ck, cv = ka.shape[1], ka.shape[1] + kb.shape[1]
    own_kv = kv_all.at[sp_me]
    own = [
        (ka, own_kv.at[:, pl.ds(0, ck)]),
        (kb, own_kv.at[:, pl.ds(ck, kb.shape[1])]),
        (va, own_kv.at[:, pl.ds(cv, hv)]),
        (vb, own_kv.at[:, pl.ds(cv + hv, hv)]),
        (wd.at[pl.ds(pl.multiple_of(side * half, half), half)], wd_all.at[sp_me]),
        (oa, out_all.at[tp_me, pl.ds(0, hv)]),
        (ob, out_all.at[tp_me, pl.ds(hv, hv)]),
    ]
    copies = [pltpu.make_async_copy(s, d, local_sem.at[i]) for i, (s, d) in enumerate(own)]
    for c in copies:
        c.start()

    barrier = pltpu.get_barrier_semaphore()
    for target in list(targets) + [flip(sp_me, bit) for bit in bits]:
        pl.semaphore_signal(barrier, inc=1, device_id={"sp": target}, device_id_type=MESH)
    for peer in peers:
        pl.semaphore_signal(barrier, inc=1, device_id={"tp": peer}, device_id_type=MESH)
    for c in copies:
        c.wait()
    pl.semaphore_wait(barrier, 2 + len(bits) + len(peers))

    def piece(c, d, t, dist):
        owner = ring_to_sp((pos + n - dist) % n if d == 0 else (pos + dist) % n, n)
        part = rows // (2 * CHUNKS)
        view = kv_all.at[owner, pl.ds((d * CHUNKS + c) * part, part)]
        return pltpu.make_async_remote_copy(
            src_ref=view, dst_ref=view,
            send_sem=ring_send.at[c, d, t], recv_sem=ring_recv.at[c, d, t],
            device_id={"sp": targets[d]}, device_id_type=MESH,
        )

    for c in range(CHUNKS):
        for d in range(2):
            piece(c, d, 0, 0).start()

    tp_bits = []
    while (tp >> (len(tp_bits) + 1)) > 0:
        tp_bits.append(tp >> (len(tp_bits) + 1))
    tp_order, tp_came = [0], {}
    for k, bit in enumerate(tp_bits):
        for held in list(tp_order):
            tp_came[held | bit] = (held, k)
            tp_order.append(held | bit)

    def tp_copy(gather, held, k, arriving):
        view, first, sends, recvs = gather
        mask = held | tp_bits[k]
        dst = view(flip_all(tp_me, mask if arriving else held))
        return pltpu.make_async_remote_copy(
            src_ref=first if first is not None and held == 0 and not arriving else dst, dst_ref=dst,
            send_sem=sends.at[mask - 1], recv_sem=recvs.at[mask - 1],
            device_id={"tp": flip(tp_me, tp_bits[k])}, device_id_type=MESH,
        )

    def tp_forward(gather, mask):
        for k in range(tp_came[mask][1] + 1 if mask else 0, len(tp_bits)):
            tp_copy(gather, mask, k, False).start()

    def tp_arrive(gather, masks):
        for mask in masks:
            held, k = tp_came[mask]
            tp_copy(gather, held, k, True).wait_recv()
            tp_forward(gather, mask)

    def tp_drain(gather):
        for mask in tp_order[1:]:
            held, k = tp_came[mask]
            tp_copy(gather, held, k, False).wait_send()

    out_gather = (lambda slot: out_all.at[slot], None, out_send, out_recv)
    head_gather = (lambda slot: heads_all.at[slot], mine, head_send, head_recv)
    norm_gather = (lambda slot: normed.at[1 - side, slot], None, norm_send, norm_recv)
    tp_forward(out_gather, 0)

    tile = math.gcd(units, 128)

    def turn(i):
        at = pl.ds(pl.multiple_of(i * tile, tile), tile)
        wg_turn[at, :] = wg[:, at].T
        wu_turn[at, :] = wu[:, at].T

    turns = units // tile
    per = -(-turns // (n - 1))

    def circulate(t, _):
        for c in range(CHUNKS):
            for d in range(2):
                piece(c, d, t, t + 1).wait_recv()

                @pl.when(t + 1 < n - 1)
                def _():
                    piece(c, d, t + 1, t + 1).start()

        for k in range(per):
            @pl.when(t * per + k < turns)
            def _():
                turn(t * per + k)

        return 0

    lax.fori_loop(0, n - 1, circulate, 0)
    wg_all[sp_me] = wg_turn[pl.ds(pl.multiple_of(side * half, half), half), :]
    wu_all[sp_me] = wu_turn[pl.ds(pl.multiple_of(side * half, half), half), :]

    gathered = (wg_all, wu_all, wd_all)
    whole = (wg_turn, wu_turn, wd)

    def cube(a, held, k, arriving):
        mask = held | bits[k]
        owner = flip_all(sp_me, mask if arriving else held)
        dst = gathered[a].at[owner]
        src = dst
        if k == 0 and not arriving:
            src = whole[a].at[pl.ds(pl.multiple_of((1 - side) * half, half), half)]
        return pltpu.make_async_remote_copy(
            src_ref=src, dst_ref=dst,
            send_sem=cube_send.at[a, mask], recv_sem=cube_recv.at[a, mask],
            device_id={"sp": flip(sp_me, bits[k])}, device_id_type=MESH,
        )

    order = [0]
    came = {}
    for k, bit in enumerate(bits):
        for held in list(order):
            came[held | bit] = (held, k)
            order.append(held | bit)

    def forward(a, mask, least=0, most=len(bits)):
        first = came[mask][1] + 1 if mask else 0
        for k in range(max(first, least), most):
            cube(a, mask, k, False).start()

    def arrive(a, mask):
        held, k = came[mask]
        cube(a, held, k, True).wait_recv()
        forward(a, mask)

    forward(0, 0)
    forward(1, 0)
    forward(2, 0, least=2)
    events = []
    for k in range(len(bits)):
        for a in range(3):
            for mask in order[1:]:
                if came[mask][1] == k:
                    events.append((a, mask))

    def take(chosen):
        for a, mask in chosen:
            arrive(a, mask)
            events.remove((a, mask))

    def attend(group, r):
        queries = qa if group == 0 else qb
        size = sa if group == 0 else sb
        base = 0 if group == 0 else ck
        factor = size ** (-0.5) * math.log2(math.e)
        at = pl.ds(pl.multiple_of(r * block, block), block)
        for h in range(heads):
            start = 2 * h * size
            query = queries[at, start : start + 2 * size]
            value = kv_all[:, :, cv + group * hv + h * vd : cv + group * hv + (h + 1) * vd].reshape(total, vd)
            lanes = lax.broadcasted_iota(jnp.int32, query.shape, 1)
            ratios = []
            for j in range(2):
                if size % 128 == 0:
                    q = query[:, j * size : (j + 1) * size]
                    low = base + start + j * size
                    key = kv_all[:, :, low : low + size].reshape(total, size)
                else:
                    q = jnp.where(lanes // size == j, query, jnp.zeros_like(query))
                    low = base + start
                    key = kv_all[:, :, low : low + 2 * size].reshape(total, 2 * size)
                scores = lax.dot_general(q, key, NT, preferred_element_type=jnp.float32)
                peak = jnp.max(scores, axis=1, keepdims=True)
                weights = jnp.exp2((scores - peak) * factor)
                denom = jnp.sum(weights, axis=1, keepdims=True)
                numer = jnp.dot(weights.astype(jnp.bfloat16), value, preferred_element_type=jnp.float32)
                ratios.append(numer / denom)
            mixed = ratios[0] - lam[group, h] * ratios[1]
            inverse = lax.rsqrt(jnp.mean(mixed * mixed, axis=-1, keepdims=True) + eps_norm)
            result = mixed * inverse * gain[group : group + 1, :] * head_scale
            col = group * hv + h * vd
            mine[at, col : col + vd] = result.astype(jnp.bfloat16)

    early = [(a, mask) for a, mask in events if a < 2 and came[mask][1] < 2]
    portion = -(-len(early) // (2 * CUTS))
    cuts = [nb * i // CUTS for i in range(CUTS + 1)]
    for group in range(2):
        for i in range(CUTS):
            def body(r, _, group=group):
                attend(group, r)
                return 0

            lax.fori_loop(cuts[i], cuts[i + 1], body, 0)
            take(early[:portion])
            early = early[portion:]
            if group == 0 and i == 0:
                tp_arrive(out_gather, tp_order[1:-1])
            if group == 0 and i == 1:
                tp_arrive(out_gather, tp_order[-1:])

    tp_forward(head_gather, 0)
    tp_arrive(head_gather, tp_order[1:])
    heads_all[tp_me] = mine[...]

    def project(r, _):
        at = pl.ds(pl.multiple_of(r * block, block), block)
        acc = residual[at, :].astype(jnp.float32)
        for d in range(tp):
            acc = acc + jnp.dot(heads_all[d, at, :], out_all[d], preferred_element_type=jnp.float32)
        inverse = lax.rsqrt(jnp.mean(acc * acc, axis=-1, keepdims=True) + eps_norm)
        scaled = (acc * inverse * ngain[...]).astype(jnp.bfloat16)
        for d in range(tp):
            normed[side, d, at, :] = scaled[:, d * share : (d + 1) * share]
            summed[d, at, :] = acc[:, d * share : (d + 1) * share].astype(summed.dtype)
        return 0

    lax.fori_loop(0, nb, project, 0)

    def swap(arriving):
        there = 1 - side if arriving else side
        view = normed.at[there, tp_me]
        return pltpu.make_async_remote_copy(
            src_ref=view, dst_ref=view, send_sem=swap_sem.at[0], recv_sem=swap_sem.at[1],
            device_id={"sp": mate}, device_id_type=MESH,
        )

    swap(False).start()
    forward(2, 0, most=2)
    take([e for e in events if e[0] == 2 and came[e[1]][1] == 0])
    swap(True).wait_recv()
    tp_forward(norm_gather, 0)
    tp_arrive(norm_gather, tp_order[1:-1])
    take([e for e in events if e[0] < 2])

    step_cols = share // depth

    def feed(where):
        gate = jnp.zeros((rows, half), jnp.float32)
        upward = jnp.zeros((rows, half), jnp.float32)
        for s in range(n):
            low = (s % step_cols) * depth
            x = normed[where, s // step_cols, :, low : low + depth]
            gate = gate + lax.dot_general(x, wg_all[s], NT, preferred_element_type=jnp.float32)
            upward = upward + lax.dot_general(x, wu_all[s], NT, preferred_element_type=jnp.float32)
        hidden[where] = (gate / (1.0 + jnp.exp(-gate)) * upward).astype(jnp.bfloat16)

    def feed_one(i, _):
        @pl.when(i == 1)
        def _():
            tp_arrive(norm_gather, tp_order[-1:])

        feed((side + i) % 2)
        return 0

    lax.fori_loop(0, 2, feed_one, 0)
    take(list(events))

    cols = wd_all.shape[2]
    ratio = share // cols
    low_bit = tp_me % 2

    def block_sum(d, where):
        return [
            jnp.dot(hidden[where], wd_all[d * ratio + s], preferred_element_type=jnp.float32)
            for s in range(ratio)
        ]

    used, pending = 0, []

    def send(src, dst, **target):
        nonlocal used
        copy = pltpu.make_async_remote_copy(
            src_ref=src, dst_ref=dst, send_sem=red_send.at[used], recv_sem=red_recv.at[used],
            device_id=target, device_id_type=MESH,
        )
        copy.start()
        pending.append(copy)
        used += 1

    for i in range(2):
        for m in range(tp // 2):
            d = 2 * m + (1 - low_bit if i == 0 else low_bit)
            for where in range(2):
                for s, value in enumerate(block_sum(d, where)):
                    if i == 0:
                        sbuf[2 * m + where, :, s * cols : (s + 1) * cols] = value.astype(jnp.bfloat16)
                    else:
                        channel[2 * m + where, :, s * cols : (s + 1) * cols] = value
                if i == 0:
                    send(sbuf.at[2 * m + where], rbuf.at[2 * m + where], tp=flip(tp_me, 1))
    for m in range(tp):
        pending[m].wait_recv()
        channel[m] = channel[m] + rbuf[m].astype(jnp.float32)

    strip = rows // 2
    sent = 0
    states = [{"bit": 2, "mate": False}, {"bit": 2, "mate": False}]
    stages = len(tp_bits)
    for stage in range(stages):
        batch = []
        for lower in range(2):
            state = states[lower]
            at = pl.ds(lower * strip, strip)
            bit = state["bit"]
            moves = []
            if stage == (0 if lower else stages - 1):
                for q in range(tp // bit):
                    d = (tp_me % bit + bit * q) // 2
                    moves.append((2 * d + 1 - side, 2 * d + side))
                state["mate"] = True
                target = {"sp": mate}
            else:
                flag = (tp_me // bit) % 2
                for m in range(tp // (2 * bit)):
                    give = (tp_me % bit + bit * (1 - flag) + 2 * bit * m) // 2
                    keep = (tp_me % bit + bit * flag + 2 * bit * m) // 2
                    for where in [side] if state["mate"] else [1 - side, side]:
                        moves.append((2 * give + where, 2 * keep + where))
                state["bit"] = 2 * bit
                target = {"tp": flip(tp_me, bit)}
            for give, keep in moves:
                tbuf[sent] = channel[give, at, :].astype(jnp.bfloat16)
                batch.append((used, sent, keep, at))
                send(tbuf.at[sent], ubuf.at[sent], **target)
                sent += 1
        for index, slot, keep, at in batch:
            pending[index].wait_recv()
            channel[keep, at, :] = channel[keep, at, :] + ubuf[slot].astype(jnp.float32)
    final = channel[2 * (tp_me // 2) + side]
    out[...] = (summed[tp_me] + 0.5 * final).astype(jnp.bfloat16)

    for copy in pending:
        copy.wait_send()
    swap(False).wait_send()
    for gather in (out_gather, head_gather, norm_gather):
        tp_drain(gather)
    for a in range(3):
        for mask in order[1:]:
            held, k = came[mask]
            cube(a, held, k, False).wait_send()

    def drain(t, _):
        for c in range(CHUNKS):
            for d in range(2):
                piece(c, d, t, t).wait_send()
        return 0

    lax.fori_loop(0, n - 1, drain, 0)


def local(
    n, tp, residual, queries_a, keys_a, values_a, queries_b, keys_b, values_b, mix_lambda, head_gain,
    out_a, out_b, norm_gain, w_gate, w_up, w_down,
):
    rows, width = residual.shape
    share = width // tp
    units = w_gate.shape[1]
    hv = out_a.shape[0]
    span = keys_a.shape[1] + keys_b.shape[1] + values_a.shape[1] + values_b.shape[1]
    vmem, anywhere = pl.BlockSpec(memory_space=pltpu.VMEM), pl.BlockSpec(memory_space=pl.ANY)
    smem = pl.BlockSpec(memory_space=pltpu.SMEM)
    bf16, f32 = jnp.bfloat16, jnp.float32
    dma = pltpu.SemaphoreType.DMA
    return pl.pallas_call(
        functools.partial(kernel, n, tp),
        out_shape=jax.ShapeDtypeStruct((rows, share), bf16),
        in_specs=[
            vmem, vmem, anywhere, anywhere, vmem, anywhere, anywhere, smem, vmem,
            anywhere, anywhere, vmem, vmem, vmem, anywhere,
        ],
        out_specs=vmem,
        scratch_shapes=[
            pltpu.VMEM((n, rows, span), bf16),
            pltpu.VMEM((units, w_gate.shape[0]), bf16),
            pltpu.VMEM((units, w_gate.shape[0]), bf16),
            pltpu.VMEM((n, units // 2, w_gate.shape[0]), bf16),
            pltpu.VMEM((n, units // 2, w_gate.shape[0]), bf16),
            pltpu.VMEM((n, units // 2, w_down.shape[1]), bf16),
            pltpu.VMEM((tp, 2 * hv, width), bf16),
            pltpu.VMEM((tp, rows, 2 * hv), bf16),
            pltpu.VMEM((tp, rows, share), f32),
            pltpu.VMEM((2, tp, rows, share), bf16),
            pltpu.VMEM((2, rows, units // 2), bf16),
            pltpu.VMEM((tp, rows, share), f32),
            pltpu.VMEM((tp, rows, share), bf16),
            pltpu.VMEM((tp, rows, share), bf16),
            pltpu.VMEM((2 * (tp - 1), rows // 2, share), bf16),
            pltpu.VMEM((2 * (tp - 1), rows // 2, share), bf16),
            pltpu.VMEM((rows, 2 * hv), bf16),
            dma((7,)),
            dma((CHUNKS, 2, n - 1)),
            dma((CHUNKS, 2, n - 1)),
            dma((3, n)),
            dma((3, n)),
            dma((tp - 1,)),
            dma((tp - 1,)),
            dma((tp - 1,)),
            dma((tp - 1,)),
            dma((2,)),
            dma((tp - 1,)),
            dma((tp - 1,)),
            dma((3 * tp - 2,)),
            dma((3 * tp - 2,)),
        ],
        compiler_params=pltpu.CompilerParams(
            collective_id=0, has_side_effects=True, vmem_limit_bytes=63 * 1024 * 1024
        ),
        name="layer",
    )(
        residual, queries_a, keys_a, values_a, queries_b, keys_b, values_b, mix_lambda, head_gain,
        out_a, out_b, norm_gain.reshape(1, -1), w_gate, w_up, w_down,
    )


def solution(mesh):
    in_specs = (
        P("sp", None),
        P("sp", "tp"),
        P("sp", "tp"),
        P("sp", "tp"),
        P("sp", "tp"),
        P("sp", "tp"),
        P("sp", "tp"),
        P(None, "tp"),
        P(),
        P("tp", None),
        P("tp", None),
        P(),
        P("sp", "tp"),
        P("sp", "tp"),
        P("tp", "sp"),
    )
    body = functools.partial(local, mesh.shape["sp"], mesh.shape["tp"])
    return jax.shard_map(body, mesh=mesh, in_specs=in_specs, out_specs=P("sp", "tp"), check_vma=False)
```
